256 devices in a mesh: sp: 128 (over z, y, x), tp: 2 (over core).
Axes of the slice: x: 4, y: 4, z: 8, core: 2. Of those that a mesh axis runs over, the one named last changes fastest.
Arguments:
- tokens: bfloat16 [49152, 2048], P('sp', 'tp'), may hold values from -1620 to 1620
- input_norm_gain: float32 [2048], replicated, may hold values from 0.1 to 1.9
- outer_gate_weight: bfloat16 [2048, 1024], P(None, 'tp'), may hold values from -0.125 to 0.125
- inner_gate_weight: bfloat16 [2048, 1024], P(None, 'tp'), may hold values from -0.125 to 0.125
- convolution_input_weight: bfloat16 [2048, 1024], P(None, 'tp'), may hold values from -0.125 to 0.125
- convolution_kernel_taps: bfloat16 [3, 1024], P(None, 'tp'), may hold values from -3 to 3
- query_weight_matrix: bfloat16 [2048, 512], P(None, 'tp'), may hold values from -0.125 to 0.125
- key_weight_matrix: bfloat16 [2048, 512], P(None, 'tp'), may hold values from -0.125 to 0.125
- value_weight_matrix: bfloat16 [2048, 1024], P(None, 'tp'), may hold values from -0.125 to 0.125
- forget_gate_weight: bfloat16 [2048, 512], P(None, 'tp'), may hold values from -0.125 to 0.125
- attention_gate_weight: bfloat16 [2048, 1024], P(None, 'tp'), may hold values from -0.125 to 0.125
- forget_gate_bias: float32 [512], P('tp'), may hold values from -1.5 to 10
- extra_logarithm_decay: float32 [49152, 16], P('sp', 'tp'), may hold values from -0.72 to 0
- initial_head_state: float32 [16, 32, 64], P('tp'), may hold values from -768 to 768
- head_norm_gain: float32 [64], replicated, may hold values from 0.1 to 1.9
- convolution_output_weight: bfloat16 [1024, 2048], P('tp'), may hold values from -0.125 to 0.125
- attention_output_weight: bfloat16 [1024, 2048], P('tp'), may hold values from -0.125 to 0.125
Outputs:
- mixed: bfloat16 [49152, 2048], P(('sp', 'tp'))
The draws below stay inside these ranges and needn't reach their ends.
All inputs are finite; a program needn't handle non-finite values.
Results may differ from the reference program's by a relative error of at most 0.017.
Values may be sent and summed in bfloat16 or wider, within the bound.
A program may use at most 128 MiB of HBM per device.

```python
import math
import jax
import jax.numpy as jnp
from jax import lax

D = 2048
CW = 1024
HEADS = 16
DK = 32
DV = 64
CONV_K = 3
BLOCK = 64
TOK_DEV = 384
TOKENS = 49152


def draw_tokens(key, part):
    noise_key, row_key, col_key = jax.random.split(jax.random.fold_in(key, 11), 3)
    noise = jax.random.truncated_normal(noise_key, -6.0, 6.0, (TOKENS, D), jnp.float32)
    row_scale = jnp.exp(jax.random.uniform(row_key, (TOKENS, 1), jnp.float32) * math.log(10.0))
    ramp = jnp.arange(D, dtype=jnp.float32) / max(D - 1, 1)
    rise = math.log(3.0)
    col_scale = jnp.exp(rise * ramp[None, :] + jax.random.uniform(col_key, (1, D), jnp.float32) * math.log(3.0))
    return (noise * row_scale * col_scale).astype(jnp.bfloat16)


def draw_forget_gate_bias(key, part):
    kind_key, slow_key, fast_key, jitter_key = jax.random.split(jax.random.fold_in(key, 23), 4)
    order = jax.random.permutation(kind_key, HEADS)
    fast_count = HEADS // 2
    is_fast = (order < fast_count)[:, None]
    slow = jax.random.uniform(slow_key, (HEADS, 1), jnp.float32, 8.0, 9.5)
    fast = jax.random.uniform(fast_key, (HEADS, 1), jnp.float32, -1.0, 1.0)
    jitter = jax.random.uniform(jitter_key, (HEADS, DK), jnp.float32, -0.5, 0.5)
    return (jnp.where(is_fast, fast, slow) + jitter).reshape(HEADS * DK)


def draw_extra_logarithm_decay(key, part):
    rate_key, hit_key, size_key = jax.random.split(jax.random.fold_in(key, 37), 3)
    device_blocks = TOKENS // TOK_DEV
    spread = jax.random.uniform(rate_key, (device_blocks, HEADS), jnp.float32) * math.log(4.0)
    per_row = jnp.repeat(5e-06 * jnp.exp(spread), TOK_DEV, axis=0)
    hits = jax.random.randint(hit_key, (TOKENS, HEADS), 0, TOKENS) < 2
    sizes = jax.random.uniform(size_key, (TOKENS, HEADS), jnp.float32, math.log(0.5), math.log(0.8))
    return -per_row + jnp.where(hits, sizes, 0.0)


def block_scale(rng, dims, pieces, least, top_value):
    gain = 1.0
    for axis_at, parts in pieces:
        heights = jax.random.uniform(jax.random.fold_in(jax.random.fold_in(rng, 6), axis_at), (parts,), jnp.float32, least / len(pieces), top_value / len(pieces))
        gain = gain * jnp.repeat(jnp.exp(heights), dims[axis_at] // parts).reshape((-1,) + (1,) * (len(dims) - 1 - axis_at))
    return gain


def bell_draw(rng, shape, deviation, most, cuts=(), kind=jnp.bfloat16):
    level = block_scale(rng, shape, cuts, -0.22, 0.18) if cuts else 1.0
    result = jax.random.normal(rng, shape, jnp.float32) * deviation * level
    return jnp.minimum(jnp.maximum(result, -most), most).astype(kind)


def setup_inputs(seed: int = 0) -> dict:
    seeds = jax.random.split(jax.random.key(seed), 18)
    return {
        "tokens": draw_tokens(jax.random.fold_in(seeds[17], 71), 0),
        "input_norm_gain": jnp.clip(1.0 + 0.18 * jax.random.normal(seeds[1], (D,), jnp.float32), 0.1, 1.9),
        "outer_gate_weight": bell_draw(seeds[2], (D, CW), D ** -0.5, 0.125, ((1, 2),)),
        "inner_gate_weight": bell_draw(seeds[3], (D, CW), D ** -0.5, 0.125, ((1, 2),)),
        "convolution_input_weight": bell_draw(seeds[4], (D, CW), D ** -0.5, 0.125, ((1, 2),)),
        "convolution_kernel_taps": bell_draw(seeds[5], (CONV_K, CW), 0.577, 3.0, ((1, 2),)),
        "query_weight_matrix": bell_draw(seeds[6], (D, HEADS * DK), D ** -0.5, 0.125, ((1, 2),)),
        "key_weight_matrix": bell_draw(seeds[7], (D, HEADS * DK), D ** -0.5, 0.125, ((1, 2),)),
        "value_weight_matrix": bell_draw(seeds[8], (D, HEADS * DV), D ** -0.5, 0.125, ((1, 2),)),
        "forget_gate_weight": bell_draw(seeds[9], (D, HEADS * DK), D ** -0.5, 0.125, ((1, 2),)),
        "attention_gate_weight": bell_draw(seeds[10], (D, HEADS * DV), D ** -0.5, 0.125, ((1, 2),)),
        "forget_gate_bias": draw_forget_gate_bias(jax.random.fold_in(seeds[17], 71), 0),
        "extra_logarithm_decay": draw_extra_logarithm_decay(jax.random.fold_in(seeds[17], 71), 0),
        "initial_head_state": bell_draw(seeds[13], (HEADS, DK, DV), 128.0, 768.0, ((0, 2),), jnp.float32),
        "head_norm_gain": jnp.clip(1.0 + 0.18 * jax.random.normal(seeds[14], (DV,), jnp.float32), 0.1, 1.9),
        "convolution_output_weight": bell_draw(seeds[15], (CW, D), (CW + HEADS * DV) ** -0.5, 0.125, ((0, 2),)),
        "attention_output_weight": bell_draw(seeds[16], (HEADS * DV, D), (CW + HEADS * DV) ** -0.5, 0.125, ((0, 2),)),
    }


NORM_EPS = 1e-06
GATE_SOFTNESS = 16.0

def block_terms(queries, key_rows, values, logarithm_decay):
    cumulative = jnp.cumsum(logarithm_decay, axis=1)
    last_log = cumulative[:, -1:]
    query_g = queries * jnp.exp(cumulative)
    key_g = key_rows * jnp.exp(-cumulative)
    scores = jnp.einsum('nihd,njhd->nhij', query_g, key_g, precision=lax.Precision.HIGHEST)
    width = queries.shape[1]
    causal = jnp.arange(width)[:, None] >= jnp.arange(width)[None, :]
    scores = jnp.where(causal, scores, 0.0)
    inner = jnp.einsum('nhij,njhe->nihe', scores, values, precision=lax.Precision.HIGHEST)
    key_decayed = key_rows * jnp.exp(last_log - cumulative)
    update = jnp.einsum('nchd,nche->nhde', key_decayed, values, precision=lax.Precision.HIGHEST)
    return (query_g, inner, update, last_log[:, 0])

def carry_step(state, inputs):
    block_decay, update = inputs
    return (block_decay[..., None] * state + update, state)

def reference(tokens, input_norm_gain, outer_gate_weight, inner_gate_weight, convolution_input_weight, convolution_kernel_taps, query_weight_matrix, key_weight_matrix, value_weight_matrix, forget_gate_weight, attention_gate_weight, forget_gate_bias, extra_logarithm_decay, initial_head_state, head_norm_gain, convolution_output_weight, attention_output_weight):
    sequence_length = tokens.shape[0]
    number_of_heads, key_channel_count, value_dim = initial_head_state.shape
    features = tokens.astype(jnp.float32)
    power = lax.optimization_barrier(jnp.mean(features * features, axis=1, keepdims=True))
    normed = (features * lax.rsqrt(power + NORM_EPS) * input_norm_gain).astype(jnp.bfloat16)

    def project(weight):
        return jnp.dot(normed, weight, preferred_element_type=jnp.float32).astype(jnp.bfloat16)
    conv_b, conv_c, conv_h = (project(outer_gate_weight), project(inner_gate_weight), project(convolution_input_weight))
    query, key_proj, value = (project(query_weight_matrix), project(key_weight_matrix), project(value_weight_matrix))
    forget_preactivation, out_gate = (project(forget_gate_weight), project(attention_gate_weight))
    product = (conv_c.astype(jnp.float32) * conv_h.astype(jnp.float32)).astype(jnp.bfloat16)
    tap_count = convolution_kernel_taps.shape[0]
    padded = jnp.concatenate([jnp.zeros((tap_count - 1, product.shape[1]), jnp.bfloat16), product], axis=0)
    conv = jnp.zeros(product.shape, jnp.float32)
    for tap_index in range(tap_count):
        conv = conv + convolution_kernel_taps[tap_index].astype(jnp.float32) * padded[tap_index:tap_index + sequence_length].astype(jnp.float32)
    conv_out = (conv_b.astype(jnp.float32) * conv).astype(jnp.bfloat16)
    logarithm_decay = jax.nn.log_sigmoid(forget_preactivation.astype(jnp.float32) + forget_gate_bias) / GATE_SOFTNESS
    logarithm_decay = logarithm_decay.reshape(sequence_length, number_of_heads, key_channel_count) + extra_logarithm_decay[:, :, None]
    n_blocks = sequence_length // BLOCK
    queries = (query.astype(jnp.float32) * key_channel_count ** (-0.5)).reshape(n_blocks, BLOCK, number_of_heads, key_channel_count)
    key_rows = key_proj.astype(jnp.float32).reshape(n_blocks, BLOCK, number_of_heads, key_channel_count)
    values = value.astype(jnp.float32).reshape(n_blocks, BLOCK, number_of_heads, value_dim)
    query_g, inner, update, block_log = block_terms(queries, key_rows, values, logarithm_decay.reshape(n_blocks, BLOCK, number_of_heads, key_channel_count))
    final_state, entering = lax.scan(carry_step, initial_head_state.astype(jnp.float32), (jnp.exp(block_log), update))
    outer = jnp.einsum('nchd,nhde->nche', query_g, entering, precision=lax.Precision.HIGHEST)
    raw = (inner + outer).reshape(sequence_length, number_of_heads, value_dim)
    raw = raw * lax.rsqrt(lax.optimization_barrier(jnp.mean(raw * raw, axis=2, keepdims=True)) + NORM_EPS) * head_norm_gain
    gate_values = jax.nn.silu(out_gate.astype(jnp.float32)).reshape(sequence_length, number_of_heads, value_dim)
    attn_out = (raw * gate_values).reshape(sequence_length, number_of_heads * value_dim).astype(jnp.bfloat16)
    mixed = jnp.dot(conv_out, convolution_output_weight, preferred_element_type=jnp.float32)
    mixed = mixed + jnp.dot(attn_out, attention_output_weight, preferred_element_type=jnp.float32)
    return mixed.astype(jnp.bfloat16)
```

```python
import jax
import jax.numpy as jnp
from jax import lax
from jax.experimental import pallas as pl
from jax.experimental.pallas import tpu as pltpu
from jax.sharding import PartitionSpec as P

F32 = jnp.float32
BF16 = jnp.bfloat16
NORM_EPS = 1e-06
MESH = pl.DeviceIdType.MESH

ROWS = 384
HALF = 1024
BLK = 128
NBLK = ROWS // BLK
PLANE = 16
PLANES = 8
K0, F0, V0, C0, H0, B0, G0, Q0 = 0, 256, 512, 1024, 1536, 2048, 2560, 3072
WIDE = 3328


def split2(x):
    hi = x.astype(BF16)
    lo = (x - hi.astype(F32)).astype(BF16)
    return hi, lo


def split3(x):
    hi = x.astype(BF16)
    rest = x - hi.astype(F32)
    mid = rest.astype(BF16)
    lo = (rest - mid.astype(F32)).astype(BF16)
    return hi, mid, lo


def iota(shape, dim):
    return lax.broadcasted_iota(jnp.int32, shape, dim)


def dot(a, b):
    return jnp.dot(a, b, preferred_element_type=F32)


def dot_t(a, b):
    return lax.dot_general(a, b, (((1,), (1,)), ((), ())), preferred_element_type=F32)


def kernel(
    tok, gain, wb, wc, wh, taps, wq, wk, wv, wf, wg, bias, extra, init, hgain, wco, wao,
    out,
    X, XG, W, WO, PJ, SS, RS, GN, BI, EX, TP_, HG, ST, CUM, KG, QG, QI, QF, EN,
    P1S, P1R, EU, ED, ZS, ZR, P3S, SIN, SBD, INI, PR, CO, RAW, AO, OUT, SB, RB, OB,
    lsem, osem, tok_s, tok_r, p1_s, p1_r, z_s, z_r, p3_s, p3_r, cv_s, cv_r, ot_s, ot_r,
):
    sp = lax.axis_index("sp")
    tp = lax.axis_index("tp")
    other = 1 - tp
    z = sp // PLANE
    p = sp % PLANE
    base = sp - p
    nsp = PLANE * PLANES

    bar = pltpu.get_barrier_semaphore()

    def greet(dev):
        pl.semaphore_signal(bar, inc=1, device_id=dev, device_id_type=MESH)

    greet((sp, other))
    for o in range(1, PLANE):
        greet((base + (p + o) % PLANE, tp))
    for o in range(1, PLANES):
        greet(((z + o) % PLANES * PLANE + p, tp))
    greet(((sp + 1) % nsp, tp))
    greet(((sp + nsp - 1) % nsp, tp))

    n_local = [0]

    def fetch(src, dst):
        c = pltpu.make_async_copy(src, dst, lsem.at[n_local[0]])
        n_local[0] += 1
        c.start()
        return c

    own = pl.ds(pl.multiple_of(tp * HALF, HALF), HALF)
    oth = pl.ds(pl.multiple_of(other * HALF, HALF), HALF)
    c_tok = fetch(tok, X.at[0])
    c_gain = fetch(gain, GN)
    group = [(wk, K0, 256), (wf, F0, 256), (wv, V0, 512), (wc, C0, 512), (wh, H0, 512),
             (wb, B0, 512), (wg, G0, 512), (wq, Q0, 256)]
    c_own = [fetch(w.at[own], W.at[0, :, pl.ds(o, n)]) for w, o, n in group[:3]]
    c_bias = fetch(bias, BI)
    c_extra = fetch(extra, EX)
    c_own += [fetch(w.at[own], W.at[0, :, pl.ds(o, n)]) for w, o, n in group[3:]]
    c_oth = [fetch(w.at[oth], W.at[1, :, pl.ds(o, n)]) for w, o, n in group]
    c_init = fetch(init, ST)
    c_taps = fetch(taps, TP_)
    c_hg = fetch(hgain, HG)
    c_wco = fetch(wco, WO.at[0])
    c_wao = fetch(wao, WO.at[1])

    c_tok.wait()
    c_gain.wait()

    def prepare(slot, which):
        xs = X[slot].astype(F32)
        g = GN[:, pl.ds(pl.multiple_of(which * HALF, HALF), HALF)]
        XG[slot] = (xs * g).astype(BF16)
        return jnp.sum(xs * xs, axis=1, keepdims=True)

    ss = prepare(0, tp)
    SS[...] = jnp.broadcast_to(ss, (ROWS, 128))

    def own_half(o, n):
        PJ[:, o:o + n] = dot(XG[0], W[0, :, o:o + n])

    c_own[0].wait()
    c_own[1].wait()
    own_half(K0, 512)
    c_own[2].wait()
    own_half(V0, 512)

    pl.semaphore_wait(bar, 1 + (PLANE - 1) + (PLANES - 1) + 2)
    tok_copy = pltpu.make_async_remote_copy(
        X.at[0], X.at[1], tok_s, tok_r, device_id=(sp, other), device_id_type=MESH
    )
    tok_copy.start()

    for i, o in ((3, C0), (4, H0), (5, B0), (6, G0)):
        c_own[i].wait()
        own_half(o, 512)
    c_own[7].wait()
    own_half(Q0, 256)

    tok_copy.wait_recv()
    ss1 = prepare(1, other)
    ss_all = SS[...] + jnp.broadcast_to(ss1, (ROWS, 128))
    RS[...] = lax.rsqrt(ss_all * (1.0 / (2 * HALF)) + NORM_EPS)

    def full(o, n):
        acc = PJ[:, o:o + n] + dot(XG[1], W[1, :, o:o + n])
        r = RS[...]
        return acc * jnp.concatenate([r] * (n // 128), axis=1)

    c_oth[0].wait()
    c_oth[1].wait()
    PJ[:, K0:K0 + 512] = full(K0, 512)
    c_oth[2].wait()
    PJ[:, V0:V0 + 512] = full(V0, 512)

    c_bias.wait()
    c_extra.wait()
    ex = (iota((8, 256), 1) // 32 == iota((8, 256), 0)).astype(BF16)
    e1, e2, e3 = split3(EX[...])
    spread = dot(e1, ex) + dot(e2, ex) + dot(e3, ex)
    pre = PJ[:, F0:F0 + 256] + BI[...]
    ls = (jnp.minimum(pre, 0.0) - jnp.log1p(jnp.exp(-jnp.abs(pre)))) * (1.0 / 16.0)
    ld_hi, ld_lo = split2(ls + spread)
    low = (iota((BLK, 2 * BLK), 0) >= iota((BLK, 2 * BLK), 1) % BLK).astype(BF16)
    tot = []
    kd = []
    for n in range(NBLK):
        rows = slice(n * BLK, (n + 1) * BLK)
        c = dot(low, jnp.concatenate([ld_hi[rows], ld_lo[rows]], axis=0))
        CUM[rows] = c
        t = c[BLK - 1:BLK]
        tot.append(t)
        kd.append(PJ[rows, K0:K0 + 256] * jnp.exp(t - c))
    later = [tot[1] + tot[2], tot[2], None]
    kf = [kd[n] * jnp.exp(later[n]) if later[n] is not None else kd[n] for n in range(NBLK)]
    kft = jnp.concatenate([x.T for x in kf], axis=1).astype(BF16)
    vb = PJ[:, V0:V0 + 512].astype(BF16)
    lane_lo = iota((32, 128), 1) < 64

    tot_all = tot[0] + tot[1] + tot[2]
    rr, jj = iota((128, 256), 0), iota((128, 256), 1)
    pick = jnp.logical_and(jj // 64 == rr // 32, jj % 32 == rr % 32)
    d1, d2, d3 = split3(jnp.where(pick, jnp.broadcast_to(tot_all, (128, 256)), 0.0))
    par = ((iota((256, 128), 0) // 32) % 2 == iota((256, 128), 1) // 64).astype(BF16)
    dec = jnp.exp(dot(d1, par) + dot(d2, par) + dot(d3, par))
    for g in range(2):
        u = dot(kft[g * 128:(g + 1) * 128], vb[:, g * 256:(g + 1) * 256])
        for half in range(2):
            a = u[half * 64:half * 64 + 32, half * 128:half * 128 + 128]
            b = u[half * 64 + 32:half * 64 + 64, half * 128:half * 128 + 128]
            comp = jnp.where(lane_lo, a, b)
            for i in range(4):
                s = (g * 2 + half) * 4 + i
                P1S[s, 0:8] = comp[i * 8:i * 8 + 8]
    for s in range(PLANE):
        P1S[s, 8:16] = dec[s * 8:s * 8 + 8]

    p1 = []
    for o in range(1, PLANE):
        q = (p + o) % PLANE
        c = pltpu.make_async_remote_copy(
            P1S.at[q], P1R.at[p], p1_s.at[o], p1_r.at[p], device_id=(base + q, tp), device_id_type=MESH
        )
        c.start()
        p1.append(c)
    P1R[p] = P1S[p]

    c_oth[3].wait()
    c_oth[4].wait()
    PR[8:8 + ROWS] = full(C0, 512)
    PR[8:8 + ROWS] = PR[8:8 + ROWS] * full(H0, 512)
    cv = pltpu.make_async_remote_copy(
        PR.at[pl.ds(ROWS, 8)], PR.at[pl.ds(0, 8)], cv_s, cv_r,
        device_id=((sp + 1) % nsp, tp), device_id_type=MESH,
    )
    cv.start()
    c_oth[5].wait()
    PJ[:, B0:B0 + 512] = full(B0, 512)

    for o in range(1, PLANE):
        q = (p + o) % PLANE
        pltpu.make_async_remote_copy(
            P1S.at[q], P1R.at[q], p1_s.at[o], p1_r.at[q], device_id=(base + q, tp), device_id_type=MESH
        ).wait_recv()
    eu = jnp.zeros((8, 128), F32)
    ed = jnp.ones((8, 128), F32)
    for q in range(PLANE):
        EU[q] = eu
        ED[q] = ed
        d = P1R[q, 8:16]
        eu = d * eu + P1R[q, 0:8]
        ed = d * ed
    ZS[0:8] = eu
    ZS[8:16] = ed
    zc = []
    for o in range(1, PLANES):
        t = (z + o) % PLANES
        c = pltpu.make_async_remote_copy(
            ZS, ZR.at[z], z_s.at[o], z_r.at[z], device_id=(t * PLANE + p, tp), device_id_type=MESH
        )
        c.start()
        zc.append(c)
    ZR[z] = ZS[...]

    c_oth[6].wait()
    c_hg.wait()
    gt = full(G0, 512)
    hg = jnp.concatenate([HG[...]] * 8, axis=1)
    PJ[:, G0:G0 + 512] = gt * jax.nn.sigmoid(gt) * hg
    c_oth[7].wait()
    PJ[:, Q0:Q0 + 256] = full(Q0, 256) * (32.0 ** -0.5)

    run = None
    for n in range(NBLK):
        rows = slice(n * BLK, (n + 1) * BLK)
        c = CUM[rows]
        t, m = c[BLK - 1:BLK], c[63:64]
        q, k = PJ[rows, Q0:Q0 + 256], PJ[rows, K0:K0 + 256]
        qi = q * jnp.exp(c)
        QI[rows] = qi.astype(BF16)
        QF[rows] = (qi if run is None else qi * jnp.exp(run)).astype(BF16)
        QG[rows] = (q * jnp.exp(c - m)).astype(BF16)
        KG[rows] = (k * jnp.exp(m - c)).astype(BF16)
        run = t if run is None else run + t
    diag = (iota((128, 256), 0) // 32 == iota((128, 256), 1) // 64)
    kd0 = PJ[0:BLK, K0:K0 + 256] * jnp.exp(CUM[BLK - 1:BLK] - CUM[0:BLK])
    kd1 = PJ[BLK:2 * BLK, K0:K0 + 256] * jnp.exp(CUM[2 * BLK - 1:2 * BLK] - CUM[BLK:2 * BLK])
    kd0t = kd0.T
    kd01t = (kd0 * jnp.exp(CUM[2 * BLK - 1:2 * BLK])).T
    kd1t = kd1.T
    e2t = jnp.concatenate([kd01t, kd1t], axis=1).astype(BF16)
    e1t = kd0t.astype(BF16)
    causal = iota((BLK, 512), 0) >= iota((BLK, 512), 1) % BLK
    for g in range(2):
        kc = slice(g * 128, (g + 1) * 128)
        vc = slice(V0 + g * 256, V0 + (g + 1) * 256)
        oc = slice(g * 256, (g + 1) * 256)
        EN[0] = jnp.where(diag, dot(e1t[kc], PJ[0:BLK, vc].astype(BF16)), 0.0).astype(BF16)
        EN[1] = jnp.where(diag, dot(e2t[kc], PJ[0:2 * BLK, vc].astype(BF16)), 0.0).astype(BF16)
        for n in range(NBLK):
            rows = slice(n * BLK, (n + 1) * BLK)
            kg = KG[rows, kc].astype(F32)
            vv = PJ[rows, vc]
            kl, vl = iota((BLK, 128), 1) // 32, iota((BLK, 256), 1) // 64
            km = jnp.concatenate([jnp.where(kl == a, kg, 0.0).astype(BF16) for a in range(4)], axis=0)
            vm = jnp.concatenate([jnp.where(vl == a, vv, 0.0).astype(BF16) for a in range(4)], axis=0)
            s = jnp.where(causal, dot_t(QG[rows, kc], km), 0.0).astype(BF16)
            r = dot(s, vm)
            if n > 0:
                r = r + dot(QI[rows, kc], EN[n - 1])
            RAW[rows, oc] = r

    c_init.wait()
    for pr in range(4):
        INI[pr * 32:pr * 32 + 32] = jnp.concatenate([ST[2 * pr], ST[2 * pr + 1]], axis=1)
    for o in range(1, PLANES):
        t = (z + o) % PLANES
        pltpu.make_async_remote_copy(
            ZS, ZR.at[t], z_s.at[o], z_r.at[t], device_id=(t * PLANE + p, tp), device_id_type=MESH
        ).wait_recv()
    state = INI[pl.ds(pl.multiple_of(p * 8, 8), 8)]
    for t in range(PLANES):
        new = ZR[t, 8:16] * state + ZR[t, 0:8]
        state = jnp.where(t < z, new, state)
    for q in range(PLANE):
        P3S[q] = EU[q] + ED[q] * state
    p3 = []
    for o in range(1, PLANE):
        q = (p + o) % PLANE
        c = pltpu.make_async_remote_copy(
            P3S.at[q], SIN.at[p], p3_s.at[o], p3_r.at[p], device_id=(base + q, tp), device_id_type=MESH
        )
        c.start()
        p3.append(c)
    SIN[p] = P3S[p]

    cv.wait_recv()
    c_taps.wait()
    PR[0:8] = jnp.where(sp > 0, PR[0:8], 0.0)
    tw = TP_[...].astype(F32)
    conv = tw[0:1] * PR[6:6 + ROWS] + tw[1:2] * PR[7:7 + ROWS] + tw[2:3] * PR[8:8 + ROWS]
    CO[...] = (PJ[:, B0:B0 + 512] * conv).astype(BF16)
    c_wco.wait()
    for j in range(4):
        OUT[:, j * 512:(j + 1) * 512] = dot(CO[...], WO[0, :, j * 512:(j + 1) * 512])

    for o in range(1, PLANE):
        q = (p + o) % PLANE
        pltpu.make_async_remote_copy(
            P3S.at[q], SIN.at[q], p3_s.at[o], p3_r.at[q], device_id=(base + q, tp), device_id_type=MESH
        ).wait_recv()
    ones = (iota((256, 256), 0) // 64 == iota((256, 256), 1) // 64).astype(BF16)
    zero = jnp.zeros((32, 128), F32)
    for g in range(2):
        kc = slice(g * 128, (g + 1) * 128)
        oc = slice(g * 256, (g + 1) * 256)
        parts = []
        for half in range(2):
            s0 = (g * 2 + half) * 4
            comp = jnp.concatenate([SIN[s0 + i] for i in range(4)], axis=0)
            for lo in (True, False):
                mine = jnp.where(lane_lo if lo else jnp.logical_not(lane_lo), comp, 0.0)
                parts.append(jnp.concatenate([mine, zero] if half == 0 else [zero, mine], axis=1))
        sbd = jnp.concatenate(parts, axis=0).astype(BF16)
        raw = RAW[:, oc] + dot(QF[:, kc], sbd)
        ms = dot((raw * raw).astype(BF16), ones) * (1.0 / 64.0)
        AO[:, oc] = (raw * lax.rsqrt(ms + NORM_EPS) * PJ[:, G0 + g * 256:G0 + (g + 1) * 256]).astype(BF16)

    c_wao.wait()
    his = pl.ds(pl.multiple_of(other * 192, 64), 192)
    mine = pl.ds(pl.multiple_of(tp * 192, 64), 192)
    oc_copies = []
    for j in range(4):
        cols = slice(j * 512, (j + 1) * 512)
        SB[j] = (OUT[his, cols] + dot(AO[his], WO[1, :, cols])).astype(BF16)
        c = pltpu.make_async_remote_copy(
            SB.at[j], RB.at[j], ot_s.at[j], ot_r.at[j], device_id=(sp, other), device_id_type=MESH
        )
        c.start()
        oc_copies.append(c)
    for j in range(4):
        cols = slice(j * 512, (j + 1) * 512)
        OUT[mine, cols] = OUT[mine, cols] + dot(AO[mine], WO[1, :, cols])
    fin = []
    for j in range(4):
        cols = slice(j * 512, (j + 1) * 512)
        oc_copies[j].wait_recv()
        OB[:, cols] = (OUT[mine, cols] + RB[j].astype(F32)).astype(BF16)
        c = pltpu.make_async_copy(OB.at[:, cols], out.at[:, cols], osem.at[j])
        c.start()
        fin.append(c)
    tok_copy.wait_send()
    cv.wait_send()
    for c in p1 + zc + p3 + oc_copies:
        c.wait_send()
    for c in fin:
        c.wait()


def on_device(
    tokens, input_norm_gain, outer_gate_weight, inner_gate_weight, convolution_input_weight,
    convolution_kernel_taps, query_weight_matrix, key_weight_matrix, value_weight_matrix,
    forget_gate_weight, attention_gate_weight, forget_gate_bias, extra_logarithm_decay,
    initial_head_state, head_norm_gain, convolution_output_weight, attention_output_weight,
):
    dma, reg = pltpu.SemaphoreType.DMA, pltpu.SemaphoreType.REGULAR
    v = pltpu.VMEM
    scratch = [
        v((2, ROWS, HALF), BF16),
        v((2, ROWS, HALF), BF16),
        v((2, HALF, WIDE), BF16),
        v((2, 512, 2048), BF16),
        v((ROWS, WIDE), F32),
        v((ROWS, 128), F32),
        v((ROWS, 128), F32),
        v((1, 2048), F32),
        v((1, 256), F32),
        v((ROWS, 8), F32),
        v((3, 512), BF16),
        v((1, 64), F32),
        v((8, 32, 64), F32),
        v((ROWS, 256), F32),
        v((ROWS, 256), BF16),
        v((ROWS, 256), BF16),
        v((ROWS, 256), BF16),
        v((ROWS, 256), BF16),
        v((2, 128, 256), BF16),
        v((PLANE, 16, 128), F32),
        v((PLANE, 16, 128), F32),
        v((PLANE, 8, 128), F32),
        v((PLANE, 8, 128), F32),
        v((16, 128), F32),
        v((PLANES, 16, 128), F32),
        v((PLANE, 8, 128), F32),
        v((PLANE, 8, 128), F32),
        v((128, 256), BF16),
        v((128, 128), F32),
        v((ROWS + 8, 512), F32),
        v((ROWS, 512), BF16),
        v((ROWS, 512), F32),
        v((ROWS, 512), BF16),
        v((ROWS, 2048), F32),
        v((4, 192, 512), BF16),
        v((4, 192, 512), BF16),
        v((192, 2048), BF16),
        dma((25,)), dma((4,)), dma, dma,
        dma((PLANE,)), dma((PLANE,)), dma((PLANES,)), dma((PLANES,)), dma((PLANE,)), dma((PLANE,)),
        dma, dma, dma((4,)), dma((4,)),
    ]
    return pl.pallas_call(
        kernel,
        out_shape=jax.ShapeDtypeStruct((192, 2048), BF16),
        in_specs=[pl.BlockSpec(memory_space=pl.ANY)] * 17,
        out_specs=pl.BlockSpec(memory_space=pl.ANY),
        scratch_shapes=scratch,
        compiler_params=pltpu.CompilerParams(
            collective_id=0, has_side_effects=True, vmem_limit_bytes=60 * 1024 * 1024
        ),
        name="layer",
    )(
        tokens, input_norm_gain.reshape(1, -1), outer_gate_weight, inner_gate_weight,
        convolution_input_weight, convolution_kernel_taps, query_weight_matrix, key_weight_matrix,
        value_weight_matrix, forget_gate_weight, attention_gate_weight, forget_gate_bias.reshape(1, -1),
        extra_logarithm_decay, initial_head_state, head_norm_gain.reshape(1, -1),
        convolution_output_weight, attention_output_weight,
    )


def solution(mesh):
    return jax.shard_map(
        on_device,
        mesh=mesh,
        in_specs=(
            P("sp", "tp"), P(), P(None, "tp"), P(None, "tp"), P(None, "tp"), P(None, "tp"),
            P(None, "tp"), P(None, "tp"), P(None, "tp"), P(None, "tp"), P(None, "tp"),
            P("tp"), P("sp", "tp"), P("tp", None, None), P(), P("tp", None), P("tp", None),
        ),
        out_specs=P(("sp", "tp"), None),
        check_vma=False,
    )
```
